32 devices in a mesh: sp: 8 (over z, y), dp: 4 (over x, core).
Axes of the slice: x: 2, y: 2, z: 4, core: 2. Of those that a mesh axis runs over, the one named last changes fastest.
Arguments:
- tokens: bfloat16 [4, 2048, 2048], P('dp', 'sp'), may hold values from -6 to 6
- w_query: bfloat16 [2048, 2048], P('dp', 'sp'), may hold values from -0.125 to 0.125
- w_key: bfloat16 [2048, 1024], P('dp', 'sp'), may hold values from -0.125 to 0.125
- w_value: bfloat16 [2048, 1024], P('dp', 'sp'), may hold values from -0.125 to 0.125
- w_out: bfloat16 [2048, 2048], P('dp', 'sp'), may hold values from -0.25 to 0.25
- qk_gain: float32 [2, 128], replicated, may hold values from 0.9 to 24
Outputs:
- mixed_out: bfloat16 [4, 2048, 2048], P('dp', 'sp')
The draws below stay inside these ranges and needn't reach their ends.
All inputs are finite; a program needn't handle non-finite values.
Results may differ from the reference program's by a relative error of at most 0.006.
The reference program's roundings to bfloat16 on the way count: a program that leaves them out, or rounds other values in their place, can miss the bound.
Values may be sent and summed in bfloat16 or wider, within the bound.
No kernel may reach another device: no remote copies, remote signals or barrier semaphores. Data moves between devices by JAX's collectives and lax.ppermute only.
A program may use at most 64 MiB of HBM per device.

```python
import math
import jax
import jax.numpy as jnp
from jax import lax

D = 2048
HQ = 16
KV = 8
HD = 128
GRID_W = 64
SEQ = 2048
SEQS = 4


def draw_qk_gain(key, part):
    noise = jnp.clip(jax.random.normal(key, (2, HD), jnp.float32), -3.0, 3.0)
    return 2.0 * (1.0 + 0.18 * noise)


def steps_of(rng, shape, split, low, largest):
    def one(dim, parts):
        heights = jax.random.uniform(jax.random.fold_in(jax.random.fold_in(rng, 6), dim), (parts,), jnp.float32, low / len(split), largest / len(split))
        return jnp.repeat(jnp.exp(heights), shape[dim] // parts).reshape((-1,) + (1,) * (len(shape) - dim - 1))

    level = one(*split[0])
    for cut in split[1:]:
        level = level * one(*cut)
    return level


def normal_values(key, extent, width, limit, cuts=(), held_as=jnp.bfloat16):
    result = jax.random.normal(key, extent, jnp.float32) * width
    if len(cuts) > 0:
        result = steps_of(key, extent, cuts, -0.22, 0.18) * result
    return jnp.clip(result, min=-limit, max=limit).astype(held_as)


def setup_inputs(seed: int = 0) -> dict:
    streams_of = jax.random.split(jax.random.key(seed), 7)
    tokens = normal_values(streams_of[0], (SEQS, SEQ, D), 1.0, 6.0, ((0, 4), (1, 8)))
    w_query = normal_values(streams_of[1], (D, HQ * HD), D ** -0.5, 0.125, ((0, 4), (1, 8)))
    w_key = normal_values(streams_of[2], (D, KV * HD), D ** -0.5, 0.125, ((0, 4), (1, 8)))
    w_value = normal_values(streams_of[3], (D, KV * HD), D ** -0.5, 0.125, ((0, 4), (1, 8)))
    w_out = normal_values(streams_of[4], (HQ * HD, D), (HQ * HD // 4) ** -0.5, 0.25, ((0, 4), (1, 8)))
    qk_gain = draw_qk_gain(jax.random.fold_in(streams_of[6], 71), 0)
    return dict(tokens=tokens, w_query=w_query, w_key=w_key, w_value=w_value, w_out=w_out, qk_gain=qk_gain)


ROPE_BASE = 10000.0
EPS = 1e-06

def angles(positions):
    quarter = jnp.arange(0, HD // 2, 2, dtype=jnp.float32)
    inv_freq = ROPE_BASE ** (-quarter / (HD // 2))
    row_pos = (positions // GRID_W).astype(jnp.float32)
    col_pos = (positions % GRID_W).astype(jnp.float32)
    angle_table = jnp.concatenate([row_pos[:, None] * inv_freq, col_pos[:, None] * inv_freq], axis=1)
    return (jnp.cos(angle_table), jnp.sin(angle_table))

def prepare(raw_proj, gain_row, cosine, sine_table):
    normed = raw_proj * lax.rsqrt(lax.optimization_barrier(jnp.mean(raw_proj * raw_proj, axis=-1, keepdims=True)) + EPS) * gain_row
    pair_view = normed.reshape(raw_proj.shape[:-1] + (HD // 2, 2))
    first_half = pair_view[..., 0]
    second = pair_view[..., 1]
    cos_b = cosine[:, None, :]
    sin_b = sine_table[:, None, :]
    turned = jnp.stack([first_half * cos_b - second * sin_b, first_half * sin_b + second * cos_b], axis=-1)
    return turned.reshape(raw_proj.shape).astype(jnp.bfloat16)

def attend_head(query_rows, key_rows, value_rows):
    seq_len = query_rows.shape[0]
    block_len = math.gcd(seq_len, 512)
    blocks = query_rows.reshape(seq_len // block_len, block_len, HD)

    def one_block(row_block):
        scores = jnp.dot(row_block, key_rows.T, preferred_element_type=jnp.float32) * HD ** (-0.5)
        top_score = lax.optimization_barrier(jnp.max(scores, axis=1, keepdims=True))
        weights = jnp.exp(scores - top_score)
        row_total = lax.optimization_barrier(jnp.sum(weights, axis=1, keepdims=True))
        probs_bf = (weights / row_total).astype(jnp.bfloat16)
        return jnp.dot(probs_bf, value_rows, preferred_element_type=jnp.float32).astype(jnp.bfloat16)
    return lax.map(one_block, blocks).reshape(seq_len, HD)

def reference(tokens, w_query, w_key, w_value, w_out, qk_gain):
    seq_len = tokens.shape[1]
    group_size = HQ // KV
    cosine, sine_table = angles(jnp.arange(seq_len, dtype=jnp.int32))

    def one_sequence(seq_rows):
        query = prepare(jnp.dot(seq_rows, w_query, preferred_element_type=jnp.float32).reshape(seq_len, HQ, HD), qk_gain[0], cosine, sine_table)
        key_all = prepare(jnp.dot(seq_rows, w_key, preferred_element_type=jnp.float32).reshape(seq_len, KV, HD), qk_gain[1], cosine, sine_table)
        value = jnp.dot(seq_rows, w_value, preferred_element_type=jnp.float32).astype(jnp.bfloat16).reshape(seq_len, KV, HD)
        query_heads = jnp.transpose(query, (1, 0, 2))
        key_heads = jnp.repeat(jnp.transpose(key_all, (1, 0, 2)), group_size, axis=0)
        value_heads = jnp.repeat(jnp.transpose(value, (1, 0, 2)), group_size, axis=0)
        attended = lax.map(lambda triple: attend_head(triple[0], triple[1], triple[2]), (query_heads, key_heads, value_heads))
        attended = jnp.transpose(attended, (1, 0, 2)).reshape(seq_len, HQ * HD)
        return jnp.dot(attended, w_out, preferred_element_type=jnp.float32).astype(jnp.bfloat16)
    return lax.map(one_sequence, tokens)
```

```python
import functools
import math

import jax
import jax.numpy as jnp
from jax import lax
from jax.experimental import pallas as pl
from jax.experimental.pallas import tpu as pltpu
from jax.sharding import PartitionSpec as P

HQ = 16
KV = 8
HD = 128
GRID_W = 64

ROPE_BASE = 10000.0
EPS = 1e-06
LOG2E = 1.4426950408889634


def rotary_tables(seq_len):
    positions = jnp.arange(seq_len, dtype=jnp.int32)
    quarter = jnp.arange(0, HD // 2, 2, dtype=jnp.float32)
    inv_freq = jnp.repeat(ROPE_BASE ** (-quarter / (HD // 2)), 2)
    row_pos = (positions // GRID_W).astype(jnp.float32)
    col_pos = (positions % GRID_W).astype(jnp.float32)
    angle = jnp.concatenate([row_pos[:, None] * inv_freq, col_pos[:, None] * inv_freq], axis=1)
    sign = jnp.where(jnp.arange(HD) % 2 == 0, -1.0, 1.0).astype(jnp.float32)
    return jnp.cos(angle), jnp.sin(angle) * sign


def shift(n_outer, n_inner, outer):
    pairs = []
    for a in range(n_outer):
        for b in range(n_inner):
            to = ((a + 1) % n_outer, b) if outer else (a, (b + 1) % n_inner)
            pairs.append((a * n_inner + b, to[0] * n_inner + to[1]))
    return pairs


def gather_blocks(block, axis, n_outer, n_inner):
    blocks = {(0, 0): block}
    for i in range(1, n_outer):
        blocks[i, 0] = lax.ppermute(blocks[i - 1, 0], axis, shift(n_outer, n_inner, True))
    for i in range(n_outer):
        for j in range(1, n_inner):
            blocks[i, j] = lax.ppermute(blocks[i, j - 1], axis, shift(n_outer, n_inner, False))
    return blocks


def owner_of(axis, n_outer, n_inner, i, j):
    me = lax.axis_index(axis)
    return lax.rem(me // n_inner + n_outer - i, n_outer) * n_inner + lax.rem(
        lax.rem(me, n_inner) + n_inner - j, n_inner
    )


def project_kernel(n_w, n_q, n_kv, index_ref, x_ref, gain_ref, cos_ref, sin_ref, *refs):
    w_refs = refs[:n_w]
    q_ref, k_ref, v_ref = refs[-3:]
    depth = w_refs[0].shape[0]
    total = None
    for slot in range(n_w):
        columns = pl.ds(pl.multiple_of(index_ref[1 + slot] * depth, depth), depth)
        part = jnp.dot(x_ref[:, columns], w_refs[slot][...], preferred_element_type=jnp.float32)
        total = part if total is None else total + part
    cos, sin = cos_ref[...], sin_ref[...]
    even = lax.broadcasted_iota(jnp.int32, cos.shape, 1) % 2 == 0

    def turned(raw, gain):
        normed = raw * lax.rsqrt(jnp.mean(raw * raw, axis=-1, keepdims=True) + EPS) * gain
        other = jnp.where(even, pltpu.roll(normed, HD - 1, 1), pltpu.roll(normed, 1, 1))
        return (normed * cos + other * sin).astype(jnp.bfloat16)

    for h in range(n_q):
        q_ref[:, h * HD : (h + 1) * HD] = turned(total[:, h * HD : (h + 1) * HD], gain_ref[0:1, :])
    for h in range(n_kv):
        at = (n_q + h) * HD
        k_ref[:, h * HD : (h + 1) * HD] = turned(total[:, at : at + HD], gain_ref[1:2, :])
    v_ref[...] = total[:, (n_q + n_kv) * HD :].astype(jnp.bfloat16)


def project(block, weights, w_owner, position, gain, cos, sin, held, seq_len, n_q, n_kv):
    rows, depth = block.shape
    index = jnp.stack([position, *w_owner]).astype(jnp.int32)
    whole = lambda shape: pl.BlockSpec(shape, lambda i, ix: (0,) * len(shape))
    at_rows = lambda width: pl.BlockSpec((rows, width), lambda i, ix: (ix[0], 0))
    n_w = len(weights)
    width = weights[0].shape[1]
    in_specs = [whole((rows, depth)), whole(gain.shape), at_rows(HD), at_rows(HD)]
    in_specs += [whole(w.shape) for w in weights]
    args = [block, gain, cos, sin, *weights]
    aliases = {}
    if held is not None:
        in_specs += [pl.BlockSpec(memory_space=pl.ANY)] * 3
        aliases = {1 + len(args) + i: i for i in range(3)}
        args += list(held)
    return pl.pallas_call(
        functools.partial(project_kernel, n_w, n_q, n_kv),
        out_shape=[
            jax.ShapeDtypeStruct((seq_len, n_q * HD), jnp.bfloat16),
            jax.ShapeDtypeStruct((seq_len, n_kv * HD), jnp.bfloat16),
            jax.ShapeDtypeStruct((seq_len, n_kv * HD), jnp.bfloat16),
        ],
        grid_spec=pltpu.PrefetchScalarGridSpec(
            num_scalar_prefetch=1,
            grid=(1,),
            in_specs=in_specs,
            out_specs=[at_rows(n_q * HD), at_rows(n_kv * HD), at_rows(n_kv * HD)],
        ),
        input_output_aliases=aliases,
        cost_estimate=pl.CostEstimate(
            flops=2 * rows * depth * width,
            bytes_accessed=2 * (rows * depth + depth * width + rows * width),
            transcendentals=0,
        ),
        name="project",
    )(index, *args)


def attend_kernel(n_q, group, q_ref, k_ref, v_ref, o_ref):
    for h in range(n_q):
        at = (h // group) * HD
        q = q_ref[:, h * HD : (h + 1) * HD]
        scores = lax.dot_general(
            q, k_ref[:, at : at + HD], (((1,), (1,)), ((), ())), preferred_element_type=jnp.float32
        )
        top = jnp.max(scores, axis=1, keepdims=True)
        weights = jnp.exp2((scores - top) * (HD**-0.5 * LOG2E))
        total = jnp.sum(weights, axis=1, keepdims=True)
        probs = (weights * (1.0 / total)).astype(jnp.bfloat16)
        out = jnp.dot(probs, v_ref[:, at : at + HD], preferred_element_type=jnp.float32)
        o_ref[:, h * HD : (h + 1) * HD] = out.astype(jnp.bfloat16)


def attend(query, key, value, n_q, group):
    seq_len = query.shape[0]
    rows = math.gcd(seq_len, 256)
    n_kv = key.shape[1] // HD
    return pl.pallas_call(
        functools.partial(attend_kernel, n_q, group),
        out_shape=jax.ShapeDtypeStruct(query.shape, jnp.bfloat16),
        grid=(seq_len // rows,),
        in_specs=[
            pl.BlockSpec((rows, n_q * HD), lambda i: (i, 0)),
            pl.BlockSpec((seq_len, n_kv * HD), lambda i: (0, 0)),
            pl.BlockSpec((seq_len, n_kv * HD), lambda i: (0, 0)),
        ],
        out_specs=pl.BlockSpec((rows, n_q * HD), lambda i: (i, 0)),
        cost_estimate=pl.CostEstimate(
            flops=4 * seq_len * seq_len * n_q * HD * 2,
            bytes_accessed=2 * seq_len * (2 * n_q + 2 * n_kv) * HD,
            transcendentals=seq_len * seq_len * n_q,
        ),
        name="attend",
    )(query, key, value)


def mix_kernel(keys, n_z, index_ref, a_ref, *refs):
    o_ref = refs[-1]
    w_refs = refs[:-1]
    n_d = len(w_refs)
    step = pl.program_id(0)
    total = None
    for slot in range(n_d):
        rows = w_refs[slot].shape[-2]
        parts = rows // a_ref.shape[2]
        first = index_ref[n_z + slot] * parts
        for part in range(parts):
            width = a_ref.shape[2]
            term = jnp.dot(
                a_ref[first + part],
                w_refs[slot][0, part * width : (part + 1) * width, :],
                preferred_element_type=jnp.float32,
            )
            total = term if total is None else total + term
    o_ref[...] = total.astype(jnp.bfloat16)


def on_device(tokens, w_query, w_key, w_value, w_out, qk_gain):
    own_rows = tokens[0]
    rows, depth = own_rows.shape
    n_sp, n_dp = lax.axis_size("sp"), lax.axis_size("dp")
    seq_len = rows * n_sp
    n_z = math.gcd(n_sp, 4)
    n_y = n_sp // n_z
    n_c = math.gcd(n_dp, 2)
    n_x = n_dp // n_c
    n_q = HQ // n_sp
    group = HQ // KV
    share = max(1, n_sp // KV)
    if share > 1:
        groups = [[g * share + i for i in range(share)] for g in range(n_sp // share)]
        whole_head = lambda w: lax.all_gather(w, "sp", axis=1, axis_index_groups=groups, tiled=True)
        w_key, w_value = whole_head(w_key), whole_head(w_value)
    n_kv = w_key.shape[1] // HD

    w_own = jnp.concatenate([w_query, w_key, w_value], axis=1)
    w_blocks = gather_blocks(w_own, "dp", n_x, n_c)
    d_order = list(w_blocks)
    d_owner = [owner_of("dp", n_x, n_c, i, j) for i, j in d_order]
    weights = [w_blocks[slot] for slot in d_order]

    cos, sin = rotary_tables(seq_len)
    blocks = gather_blocks(own_rows, "sp", n_z, n_y)
    held = None
    for slot in sorted(blocks, key=lambda s: s[0] + s[1]):
        held = project(
            blocks[slot], weights, d_owner, owner_of("sp", n_z, n_y, *slot),
            qk_gain, cos, sin, held, seq_len, n_q, n_kv,
        )
    query, key, value = held
    attended = attend(query, key, value, n_q, group)
    heads = lax.all_to_all(
        attended.reshape(n_sp, rows, n_q * HD), "sp", split_axis=0, concat_axis=0, tiled=True
    )

    wo_own, _ = lax.optimization_barrier((w_out, blocks[n_z - 1, 0]))
    ring = [wo_own]
    for _ in range(n_z - 1):
        ring.append(lax.ppermute(ring[-1], "sp", shift(n_z, n_y, True)))
    columns = [jnp.stack(ring)]
    for _ in range(n_y - 1):
        columns.append(lax.ppermute(columns[-1], "sp", shift(n_z, n_y, False)))
    rows_of = [gather_blocks(c, "dp", n_x, n_c) for c in columns]
    wide = w_out.shape[1]
    outs = []
    for j in range(n_y):
        index = jnp.stack(
            [owner_of("sp", n_z, n_y, i, j) for i in range(n_z)] + d_owner
        ).astype(jnp.int32)
        args = [rows_of[j][slot] for slot in d_order]
        in_specs = [pl.BlockSpec(heads.shape, lambda i, ix: (0, 0, 0))]
        in_specs += [pl.BlockSpec((1, *a.shape[1:]), lambda i, ix: (i, 0, 0)) for a in args]
        aliases = {}
        extra = []
        if outs:
            in_specs.append(pl.BlockSpec(memory_space=pl.ANY))
            extra = [outs[-1]]
            aliases = {2 + len(args): 0}
        n_d = len(args)

        def kernel(index_ref, a_ref, *refs):
            mix_kernel(None, n_z, index_ref, a_ref, *refs[:n_d], refs[-1])

        outs.append(
            pl.pallas_call(
                kernel,
                out_shape=jax.ShapeDtypeStruct((rows, wide * n_sp), jnp.bfloat16),
                grid_spec=pltpu.PrefetchScalarGridSpec(
                    num_scalar_prefetch=1,
                    grid=(n_z,),
                    in_specs=in_specs,
                    out_specs=pl.BlockSpec((rows, wide), lambda i, ix: (0, ix[i])),
                ),
                input_output_aliases=aliases,
                cost_estimate=pl.CostEstimate(
                    flops=2 * rows * depth * wide * n_z,
                    bytes_accessed=2 * depth * wide * n_z,
                    transcendentals=0,
                ),
                name="mix",
            )(index, heads, *args, *extra)
        )
    return outs[-1][None]


def solution(mesh):
    in_specs = (
        P("dp", "sp", None),
        P("dp", "sp"),
        P("dp", "sp"),
        P("dp", "sp"),
        P("dp", "sp"),
        P(),
    )
    out_specs = P("dp", "sp", None)
    return jax.shard_map(
        on_device, mesh=mesh, in_specs=in_specs, out_specs=out_specs, check_vma=False
    )
```

```python
import functools
import math

import jax
import jax.numpy as jnp
from jax import lax
from jax.experimental import pallas as pl
from jax.experimental.pallas import tpu as pltpu
from jax.sharding import PartitionSpec as P


HQ = 16
KV = 8
HD = 128
GRID_W = 64

ROPE_BASE = 10000.0
EPS = 1e-06
LOG2E = 1.4426950408889634


def rotary_tables(seq_len):
    positions = jnp.arange(seq_len, dtype=jnp.int32)
    quarter = jnp.arange(0, HD // 2, 2, dtype=jnp.float32)
    inv_freq = jnp.repeat(ROPE_BASE ** (-quarter / (HD // 2)), 2)
    row_pos = (positions // GRID_W).astype(jnp.float32)
    col_pos = (positions % GRID_W).astype(jnp.float32)
    angle = jnp.concatenate([row_pos[:, None] * inv_freq, col_pos[:, None] * inv_freq], axis=1)
    sign = jnp.where(jnp.arange(HD) % 2 == 0, -1.0, 1.0).astype(jnp.float32)
    return jnp.cos(angle), jnp.sin(angle) * sign


def shift(n_outer, n_inner, outer):
    pairs = []
    for a in range(n_outer):
        for b in range(n_inner):
            to = ((a + 1) % n_outer, b) if outer else (a, (b + 1) % n_inner)
            pairs.append((a * n_inner + b, to[0] * n_inner + to[1]))
    return pairs


def send_back(n_outer, n_inner, i, j):
    return [
        (a * n_inner + b, (a - i) % n_outer * n_inner + (b - j) % n_inner)
        for a in range(n_outer)
        for b in range(n_inner)
    ]


def owner_of(axis, n_outer, n_inner, i, j):
    me = lax.axis_index(axis)
    return lax.rem(me // n_inner + 2 * n_outer - i, n_outer) * n_inner + lax.rem(
        lax.rem(me, n_inner) + 2 * n_inner - j, n_inner
    )


def whole(shape):
    return pl.BlockSpec(shape, lambda i, ix: (0,) * len(shape))


ANY = pl.BlockSpec(memory_space=pl.ANY)


def params(mib):
    return pltpu.CompilerParams(vmem_limit_bytes=mib * 2**20)


def assemble_kernel(places, index_ref, *refs):
    block_refs, (out_ref, sem) = refs[:-2], refs[-2:]
    copies = []
    for t, (b, lead, row, col) in enumerate(places):
        src = block_refs[b] if lead is None else block_refs[b].at[lead]
        height, width = src.shape
        to = out_ref
        if row is not None:
            to = to.at[pl.ds(pl.multiple_of(index_ref[row] * height, height), height)]
        if col is not None:
            to = to.at[:, pl.ds(pl.multiple_of(index_ref[col] * width, width), width)]
        copies.append(pltpu.make_async_copy(src, to, sem.at[t]))
        copies[-1].start()
    for copy in copies:
        copy.wait()


def assemble(blocks, places, index, shape):
    return pl.pallas_call(
        functools.partial(assemble_kernel, places),
        out_shape=jax.ShapeDtypeStruct(shape, jnp.bfloat16),
        grid_spec=pltpu.PrefetchScalarGridSpec(
            num_scalar_prefetch=1,
            grid=(1,),
            in_specs=[ANY] * len(blocks),
            out_specs=whole(shape),
            scratch_shapes=[pltpu.SemaphoreType.DMA((len(places),))],
        ),
        cost_estimate=pl.CostEstimate(
            flops=1000 * math.prod(shape), bytes_accessed=4 * math.prod(shape), transcendentals=0
        ),
        compiler_params=params(8),
        name="assemble",
    )(index, *blocks)


def project_kernel(n_b, n_x, n_q, n_kv, first, index_ref, *refs):
    x_refs, refs = refs[:n_x], refs[n_x:]
    cos_refs, refs = refs[:n_b], refs[n_b:]
    sin_refs, refs = refs[:n_b], refs[n_b:]
    gain_ref, w_ref = refs[:2]
    outs, held, x_whole, x_sem, sem = refs[-9:-6], refs[-6:-3], refs[-3], refs[-2], refs[-1]
    q_ref, k_ref, v_ref = held
    loads = []
    for t in range(n_x):
        height = x_refs[t].shape[0]
        loads.append(pltpu.make_async_copy(x_refs[t], x_whole.at[pl.ds(t * height, height)], x_sem.at[t]))
        loads[-1].start()
    q_width, kv_width = n_q * HD, n_kv * HD
    even = lax.broadcasted_iota(jnp.int32, cos_refs[0].shape, 1) % 2 == 0
    rows = q_ref.shape[1]
    copies = []
    for b in range(n_b):
        for load in loads[b * n_x // n_b : (b + 1) * n_x // n_b]:
            load.wait()
        x = x_whole[b * rows : (b + 1) * rows, :]
        total = jnp.dot(x, w_ref[...], preferred_element_type=jnp.float32)
        cos, sin = cos_refs[b][...], sin_refs[b][...]

        def turned(raw, gain):
            normed = raw * lax.rsqrt(jnp.mean(raw * raw, axis=-1, keepdims=True) + EPS) * gain
            other = jnp.where(even, pltpu.roll(normed, HD - 1, 1), pltpu.roll(normed, 1, 1))
            return (normed * cos + other * sin).astype(jnp.bfloat16)

        for h in range(n_q):
            at = h * HD
            q_ref[b, :, at : at + HD] = turned(total[:, at : at + HD], gain_ref[0:1, :])
        for h in range(n_kv):
            at = h * HD
            raw = total[:, q_width + at : q_width + at + HD]
            k_ref[b, :, at : at + HD] = turned(raw, gain_ref[1:2, :])
        v_ref[b] = total[:, q_width + kv_width :].astype(jnp.bfloat16)
    for i in range(3):
        copies.append(pltpu.make_async_copy(held[i], outs[i].at[pl.ds(first, n_b)], sem.at[i]))
        copies[-1].start()
    for copy in copies:
        copy.wait()


def project(blocks, slots, first, weight, index, n_d, gain, cos, sin, n_q, n_kv, held, n_all):
    halves = [half for block in blocks for half in block]
    n_b, n_x = len(blocks), len(halves)
    depth = halves[0].shape[1]
    rows = halves[0].shape[0] * n_x // n_b
    width = weight.shape[1]
    at_rows = [pl.BlockSpec((rows, HD), lambda i, ix, s=s: (ix[n_d + s], 0)) for s in slots]
    in_specs = [ANY] * n_x + at_rows + at_rows + [whole(gain.shape), whole(weight.shape)]
    args = [*halves, *[cos] * n_b, *[sin] * n_b, gain, weight]
    aliases = {}
    if held is not None:
        aliases = {1 + len(args) + i: i for i in range(3)}
        in_specs += [ANY] * 3
        args += list(held)
    widths = (n_q * HD, n_kv * HD, n_kv * HD)
    return pl.pallas_call(
        functools.partial(project_kernel, n_b, n_x, n_q, n_kv, first),
        out_shape=[jax.ShapeDtypeStruct((n_all, rows, w), jnp.bfloat16) for w in widths],
        grid_spec=pltpu.PrefetchScalarGridSpec(
            num_scalar_prefetch=1,
            grid=(1,),
            in_specs=in_specs,
            out_specs=[ANY] * 3,
            scratch_shapes=[pltpu.VMEM((n_b, rows, w), jnp.bfloat16) for w in widths]
            + [
                pltpu.VMEM((n_b * rows, depth), jnp.bfloat16),
                pltpu.SemaphoreType.DMA((n_x,)),
                pltpu.SemaphoreType.DMA((3,)),
            ],
        ),
        input_output_aliases=aliases,
        cost_estimate=pl.CostEstimate(
            flops=4 * n_b * rows * depth * width,
            bytes_accessed=2 * (n_b * rows * depth + depth * width + n_b * rows * width),
            transcendentals=0,
        ),
        compiler_params=params(20),
        name="project",
    )(index, *args)


def attend_kernel(n_q, group, qs, keys, carried, final, q_ref, k_ref, v_ref, *refs):
    if carried:
        acc_in, ml_in = refs[:2]
    outs = refs[-(qs[1] - qs[0]) :] if final else refs[-2:]
    rows = q_ref.shape[1]
    scale = HD**-0.5 * LOG2E

    def one(b, out_ref):
        for h in range(n_q):
            at = (h // group) * HD
            cols = slice(h * HD, (h + 1) * HD)
            some = k_ref[keys[0] : keys[1], :, at : at + HD].reshape((keys[1] - keys[0]) * rows, HD)
            values = v_ref[keys[0] : keys[1], :, at : at + HD].reshape((keys[1] - keys[0]) * rows, HD)
            scores = lax.dot_general(
                q_ref[b, :, cols], some, (((1,), (1,)), ((), ())), preferred_element_type=jnp.float32
            )
            top = jnp.max(scores, axis=1, keepdims=True)
            if carried:
                top_in = ml_in[b, :, 2 * h : 2 * h + 1]
                top = jnp.maximum(top, top_in)
                fade = jnp.exp2((top_in - top) * scale)
            weights = jnp.exp2((scores - top) * scale)
            total = jnp.sum(weights, axis=1, keepdims=True)
            out = jnp.dot(weights.astype(jnp.bfloat16), values, preferred_element_type=jnp.float32)
            if carried:
                total = total + fade * ml_in[b, :, 2 * h + 1 : 2 * h + 2]
                out = out + fade * acc_in[b, :, cols]
            if final:
                out_ref[:, cols] = (out * (1.0 / total)).astype(jnp.bfloat16)
            else:
                outs[0][b, :, cols] = out
                outs[1][b, :, 2 * h : 2 * h + 1] = top
                outs[1][b, :, 2 * h + 1 : 2 * h + 2] = total

    if final:
        for b in range(*qs):
            one(b, outs[b - qs[0]])
    else:
        pl.loop(*qs)(lambda b: one(b, None))


def attend(held, state, qs, keys, carried, final, n_q, group):
    query, key, value = held
    n_all, rows, _ = query.shape
    n_kv = key.shape[2] // HD
    vmem = pl.BlockSpec(memory_space=pltpu.VMEM)
    args, in_specs, aliases = [query, key, value], [vmem] * 3, {}
    if state is not None and (carried or not final):
        in_specs += [vmem if carried else ANY] * 2
        args += list(state)
    if final:
        out_shape = [jax.ShapeDtypeStruct((rows, n_q * HD), jnp.bfloat16)] * (qs[1] - qs[0])
    else:
        out_shape = [
            jax.ShapeDtypeStruct((n_all, rows, n_q * HD), jnp.float32),
            jax.ShapeDtypeStruct((n_all, rows, 128), jnp.float32),
        ]
        if state is not None:
            aliases = {3: 0, 4: 1}
    n_pairs = (qs[1] - qs[0]) * (keys[1] - keys[0])
    return pl.pallas_call(
        functools.partial(attend_kernel, n_q, group, qs, keys, carried, final),
        out_shape=out_shape,
        in_specs=in_specs,
        out_specs=[vmem] * len(out_shape),
        input_output_aliases=aliases,
        cost_estimate=pl.CostEstimate(
            flops=16 * n_pairs * rows * rows * n_q * HD,
            bytes_accessed=2 * (qs[1] - qs[0]) * rows * (2 * n_q + 2 * n_kv) * HD,
            transcendentals=n_pairs * rows * rows * n_q,
        ),
        compiler_params=params(24),
        name="attend",
    )(*args)


def mix_kernel(places, n_s, n_y, n_d, index_ref, *refs):
    a_refs, w_refs = refs[:n_s], refs[n_s:-3]
    o_ref, a_held, a_whole = refs[-3:]
    _, part = a_refs[0].shape
    depth, wide = w_refs[0].shape[-2:]
    many = depth // part
    for s in range(n_s):
        a_held[index_ref[n_d + 2 * n_s + s]] = a_refs[s][...]
    for d in range(n_d):
        for p in range(many):
            at = d * depth + p * part
            a_whole[:, at : at + part] = a_held[index_ref[d] * many + p]
    for i, j in sorted({(i, j) for i, j, _ in places}):
        total = None
        for d in range(n_d):
            t, plane = places[i, j, d]
            lhs = a_whole[:, d * depth : (d + 1) * depth]
            term = jnp.dot(lhs, w_refs[t][plane], preferred_element_type=jnp.float32)
            total = term if total is None else total + term
        at = pl.multiple_of(index_ref[n_d + i * n_y + j] * wide, wide)
        o_ref[:, pl.ds(at, wide)] = total.astype(jnp.bfloat16)


def mix(heads, pieces, places, index, n_y, n_d):
    n_s = len(heads)
    rows, part = heads[0].shape
    wide = pieces[0].shape[2]
    vmem = pl.BlockSpec(memory_space=pltpu.VMEM)
    return pl.pallas_call(
        functools.partial(mix_kernel, places, n_s, n_y, n_d),
        out_shape=jax.ShapeDtypeStruct((rows, n_s * wide), jnp.bfloat16),
        in_specs=[pl.BlockSpec(memory_space=pltpu.SMEM)] + [vmem] * (n_s + len(pieces)),
        out_specs=vmem,
        scratch_shapes=[
            pltpu.VMEM((n_s, rows, part), jnp.bfloat16),
            pltpu.VMEM((rows, n_s * part), jnp.bfloat16),
        ],
        cost_estimate=pl.CostEstimate(
            flops=2 * rows * n_s * part * n_s * wide,
            bytes_accessed=2 * n_s * part * n_s * wide,
            transcendentals=0,
        ),
        compiler_params=params(16),
        name="mix",
    )(index, *heads, *pieces)


def layout(n_sp, n_dp):
    n_z, n_c = math.gcd(n_sp, 4), math.gcd(n_dp, 2)
    return n_z, n_sp // n_z, n_dp // n_c, n_c


def on_device(tokens, w_query, w_key, w_value, w_out, qk_gain):
    own_rows = tokens[0]
    rows, depth = own_rows.shape
    n_sp, n_dp = lax.axis_size("sp"), lax.axis_size("dp")
    seq_len = rows * n_sp
    n_z, n_y, n_x, n_c = layout(n_sp, n_dp)
    n_q = HQ // n_sp
    group = HQ // KV
    share = max(1, n_sp // KV)
    if share > 1:
        groups = [[g * share + i for i in range(share)] for g in range(n_sp // share)]
        whole_head = lambda w: lax.all_gather(w, "sp", axis=1, axis_index_groups=groups, tiled=True)
        w_key, w_value = whole_head(w_key), whole_head(w_value)
    n_kv = w_key.shape[1] // HD
    d_slots = [(i, 0) for i in range(n_x)] + [(i, j) for i in range(n_x) for j in range(1, n_c)]
    s_slots = [(i, j) for i in range(n_z) for j in range(n_y)]
    n_d = len(d_slots)
    last = n_z + n_y - 2
    order = sorted(s_slots, key=lambda s: max(sum(s), 1))
    s_owner = {s: owner_of("sp", n_z, n_y, *s) for s in s_slots}
    index = jnp.stack(
        [owner_of("dp", n_x, n_c, *s) for s in d_slots]
        + [s_owner[s] for s in s_slots]
        + [s_owner[s] for s in order]
        + [owner_of("sp", n_z, n_y, n_z - i, n_y - j) for i, j in order]
    ).astype(jnp.int32)
    up_z, up_y = shift(n_z, n_y, True), shift(n_z, n_y, False)
    up_x, up_c = shift(n_x, n_c, True), shift(n_x, n_c, False)

    cut = rows // 2
    blocks = {(0, 0): [own_rows[:cut], lax.optimization_barrier(own_rows)[cut:]]}
    for turn in range(1, last + 1):
        for half in range(2):
            for i, j in [s for s in s_slots if sum(s) == turn]:
                before, pairs = ((i, j - 1), up_y) if j else ((i - 1, j), up_z)
                blocks.setdefault((i, j), [None, None])[half] = lax.ppermute(
                    blocks[before][half], "sp", pairs
                )

    w_blocks = {(0, 0): jnp.concatenate([w_query, w_key, w_value], axis=1)}
    for i in range(1, n_x):
        w_blocks[i, 0] = lax.ppermute(w_blocks[i - 1, 0], "dp", up_x)
    for i in range(n_x):
        for j in range(1, n_c):
            w_blocks[i, j] = lax.ppermute(w_blocks[i, j - 1], "dp", up_c)
    weight = assemble(
        [w_blocks[s] for s in d_slots],
        [(b, None, b, None) for b in range(n_d)],
        index,
        (depth, w_blocks[0, 0].shape[1]),
    )
    tables = rotary_tables(seq_len)

    held = state = None
    n_held = n_done = 0
    for turn in range(1, last + 1):
        ready = [s for s in order if max(sum(s), 1) == turn]
        held = project(
            [blocks[s] for s in ready], [s_slots.index(s) for s in ready], n_held, weight, index, n_d,
            qk_gain, *tables, n_q, n_kv, held, n_sp,
        )
        n_held += len(ready)
        old, final = (0, n_done), turn == last
        fresh = (n_done, n_held)
        carry = functools.partial(attend, n_q=n_q, group=group)
        if n_done:
            updated = carry(held, state, old, fresh, True, final)
            state = state if final else updated
        made = carry(held, state, fresh, (0, n_held), False, final)
        if final:
            attended = [*updated, *made]
        else:
            state = made
        n_done = n_held
    heads = []
    for (i, j), block in zip(order, attended):
        if i or j:
            block = lax.ppermute(block, "sp", send_back(n_z, n_y, i, j))
        heads.append(block)

    ring = [w_out]
    for _ in range(1, n_z):
        ring.append(lax.ppermute(ring[-1], "sp", up_z))
    parts = 2 if n_z % 2 == 0 else 1
    size = n_z // parts
    pieces, places = [], {}
    for k in range(parts):
        column = jnp.stack(ring[k * size : (k + 1) * size])
        for j in range(n_y):
            if j:
                column = lax.ppermute(column, "sp", up_y)
            row = column
            for i in range(n_x):
                if i:
                    row = lax.ppermute(row, "dp", up_x)
                piece = row
                for c in range(n_c):
                    if c:
                        piece = lax.ppermute(piece, "dp", up_c)
                    for p in range(size):
                        places[k * size + p, j, d_slots.index((i, c))] = len(pieces), p
                    pieces.append(piece)
    return mix(heads, pieces, places, index, n_y, n_d)[None]


def solution(mesh):
    in_specs = (
        P("dp", "sp", None),
        P("dp", "sp"),
        P("dp", "sp"),
        P("dp", "sp"),
        P("dp", "sp"),
        P(),
    )
    out_specs = P("dp", "sp", None)

    return jax.shard_map(
        on_device, mesh=mesh, in_specs=in_specs, out_specs=out_specs, check_vma=False
    )
```

```python
import functools
import math

import jax
import jax.numpy as jnp
from jax import lax
from jax.experimental import pallas as pl
from jax.experimental.pallas import tpu as pltpu
from jax.sharding import PartitionSpec as P


HQ = 16
KV = 8
HD = 128
GRID_W = 64

ROPE_BASE = 10000.0
EPS = 1e-06
LOG2E = 1.4426950408889634


def rotary_tables(seq_len):
    positions = jnp.arange(seq_len, dtype=jnp.int32)
    quarter = jnp.arange(0, HD // 2, 2, dtype=jnp.float32)
    inv_freq = jnp.repeat(ROPE_BASE ** (-quarter / (HD // 2)), 2)
    row_pos = (positions // GRID_W).astype(jnp.float32)
    col_pos = (positions % GRID_W).astype(jnp.float32)
    angle = jnp.concatenate([row_pos[:, None] * inv_freq, col_pos[:, None] * inv_freq], axis=1)
    sign = jnp.where(jnp.arange(HD) % 2 == 0, -1.0, 1.0).astype(jnp.float32)
    return jnp.cos(angle), jnp.sin(angle) * sign


def shift(n_outer, n_inner, outer):
    pairs = []
    for a in range(n_outer):
        for b in range(n_inner):
            to = ((a + 1) % n_outer, b) if outer else (a, (b + 1) % n_inner)
            pairs.append((a * n_inner + b, to[0] * n_inner + to[1]))
    return pairs


def send_back(n_outer, n_inner, i, j):
    return [
        (a * n_inner + b, (a - i) % n_outer * n_inner + (b - j) % n_inner)
        for a in range(n_outer)
        for b in range(n_inner)
    ]


def owner_of(axis, n_outer, n_inner, i, j):
    me = lax.axis_index(axis)
    return lax.rem(me // n_inner + 2 * n_outer - i, n_outer) * n_inner + lax.rem(
        lax.rem(me, n_inner) + 2 * n_inner - j, n_inner
    )


def whole(shape):
    return pl.BlockSpec(shape, lambda i, ix: (0,) * len(shape))


ANY = pl.BlockSpec(memory_space=pl.ANY)


def params(mib):
    return pltpu.CompilerParams(vmem_limit_bytes=mib * 2**20)


def assemble_kernel(places, index_ref, *refs):
    block_refs, (out_ref, sem) = refs[:-2], refs[-2:]
    copies = []
    for t, (b, lead, row, col) in enumerate(places):
        src = block_refs[b] if lead is None else block_refs[b].at[lead]
        height, width = src.shape
        to = out_ref
        if row is not None:
            to = to.at[pl.ds(pl.multiple_of(index_ref[row] * height, height), height)]
        if col is not None:
            to = to.at[:, pl.ds(pl.multiple_of(index_ref[col] * width, width), width)]
        copies.append(pltpu.make_async_copy(src, to, sem.at[t]))
        copies[-1].start()
    for copy in copies:
        copy.wait()


def assemble(blocks, places, index, shape):
    return pl.pallas_call(
        functools.partial(assemble_kernel, places),
        out_shape=jax.ShapeDtypeStruct(shape, jnp.bfloat16),
        grid_spec=pltpu.PrefetchScalarGridSpec(
            num_scalar_prefetch=1,
            grid=(1,),
            in_specs=[ANY] * len(blocks),
            out_specs=whole(shape),
            scratch_shapes=[pltpu.SemaphoreType.DMA((len(places),))],
        ),
        cost_estimate=pl.CostEstimate(
            flops=1000 * math.prod(shape), bytes_accessed=4 * math.prod(shape), transcendentals=0
        ),
        compiler_params=params(8),
        name="assemble",
    )(index, *blocks)


def project_kernel(n_b, n_x, n_q, n_kv, first, index_ref, *refs):
    x_refs, refs = refs[:n_x], refs[n_x:]
    cos_refs, refs = refs[:n_b], refs[n_b:]
    sin_refs, refs = refs[:n_b], refs[n_b:]
    gain_ref, w_ref = refs[:2]
    outs, held, x_whole, x_sem, sem = refs[-9:-6], refs[-6:-3], refs[-3], refs[-2], refs[-1]
    q_ref, k_ref, v_ref = held
    loads, ends, at = [], [], 0
    for t in range(n_x):
        height = x_refs[t].shape[0]
        loads.append(pltpu.make_async_copy(x_refs[t], x_whole.at[pl.ds(at, height)], x_sem.at[t]))
        loads[-1].start()
        at += height
        ends.append(at)
    q_width, kv_width = n_q * HD, n_kv * HD
    even = lax.broadcasted_iota(jnp.int32, cos_refs[0].shape, 1) % 2 == 0
    rows = q_ref.shape[1]
    copies = []
    for b in range(n_b):
        while ends and ends[0] <= (b + 1) * rows:
            ends.pop(0)
            loads.pop(0).wait()
        x = x_whole[b * rows : (b + 1) * rows, :]
        total = jnp.dot(x, w_ref[...], preferred_element_type=jnp.float32)
        cos, sin = cos_refs[b][...], sin_refs[b][...]

        def turned(raw, gain):
            normed = raw * lax.rsqrt(jnp.mean(raw * raw, axis=-1, keepdims=True) + EPS) * gain
            other = jnp.where(even, pltpu.roll(normed, HD - 1, 1), pltpu.roll(normed, 1, 1))
            return (normed * cos + other * sin).astype(jnp.bfloat16)

        for h in range(n_q):
            at = h * HD
            q_ref[b, :, at : at + HD] = turned(total[:, at : at + HD], gain_ref[0:1, :])
        for h in range(n_kv):
            at = h * HD
            raw = total[:, q_width + at : q_width + at + HD]
            k_ref[b, :, at : at + HD] = turned(raw, gain_ref[1:2, :])
        v_ref[b] = total[:, q_width + kv_width :].astype(jnp.bfloat16)
    for i in range(3):
        copies.append(pltpu.make_async_copy(held[i], outs[i].at[pl.ds(first, n_b)], sem.at[i]))
        copies[-1].start()
    for copy in copies:
        copy.wait()


def project(blocks, slots, first, weight, index, n_d, gain, cos, sin, n_q, n_kv, held, n_all):
    halves = [half for block in blocks for half in block]
    n_b, n_x = len(blocks), len(halves)
    depth = halves[0].shape[1]
    rows = sum(half.shape[0] for half in halves) // n_b
    width = weight.shape[1]
    at_rows = [pl.BlockSpec((rows, HD), lambda i, ix, s=s: (ix[n_d + s], 0)) for s in slots]
    in_specs = [ANY] * n_x + at_rows + at_rows + [whole(gain.shape), whole(weight.shape)]
    args = [*halves, *[cos] * n_b, *[sin] * n_b, gain, weight]
    aliases = {}
    if held is not None:
        aliases = {1 + len(args) + i: i for i in range(3)}
        in_specs += [ANY] * 3
        args += list(held)
    widths = (n_q * HD, n_kv * HD, n_kv * HD)
    return pl.pallas_call(
        functools.partial(project_kernel, n_b, n_x, n_q, n_kv, first),
        out_shape=[jax.ShapeDtypeStruct((n_all, rows, w), jnp.bfloat16) for w in widths],
        grid_spec=pltpu.PrefetchScalarGridSpec(
            num_scalar_prefetch=1,
            grid=(1,),
            in_specs=in_specs,
            out_specs=[ANY] * 3,
            scratch_shapes=[pltpu.VMEM((n_b, rows, w), jnp.bfloat16) for w in widths]
            + [
                pltpu.VMEM((n_b * rows, depth), jnp.bfloat16),
                pltpu.SemaphoreType.DMA((n_x,)),
                pltpu.SemaphoreType.DMA((3,)),
            ],
        ),
        input_output_aliases=aliases,
        cost_estimate=pl.CostEstimate(
            flops=4 * n_b * rows * depth * width,
            bytes_accessed=2 * (n_b * rows * depth + depth * width + n_b * rows * width),
            transcendentals=0,
        ),
        compiler_params=params(20),
        name="project",
    )(index, *args)


def attend_kernel(n_q, group, qs, keys, carried, final, q_ref, k_ref, v_ref, *refs):
    if carried:
        acc_old, top_old = refs[:2]
    outs = refs[-(qs[1] - qs[0]) :] if final else refs[-2:]
    rows = q_ref.shape[1]
    scale = HD**-0.5 * LOG2E

    n_keys = (keys[1] - keys[0]) * rows
    ones = jnp.ones((n_keys, HD), jnp.bfloat16)

    def one(b, out_ref):
        for h in range(n_q):
            at = (h // group) * HD
            cols = slice(h * HD, (h + 1) * HD)
            both = slice(2 * h * HD, 2 * (h + 1) * HD)
            some = k_ref[keys[0] : keys[1], :, at : at + HD].reshape(n_keys, HD)
            values = v_ref[keys[0] : keys[1], :, at : at + HD].reshape(n_keys, HD)
            scores = lax.dot_general(
                q_ref[b, :, cols], some, (((1,), (1,)), ((), ())), preferred_element_type=jnp.float32
            )
            top = jnp.broadcast_to(jnp.max(scores, axis=1, keepdims=True), (rows, HD))
            if carried:
                top_in = top_old[b, :, cols]
                top = jnp.maximum(top, top_in)
            weights = [
                jnp.exp2((scores[:, c : c + HD] - top) * scale).astype(jnp.bfloat16)
                for c in range(0, n_keys, HD)
            ]
            out = jnp.dot(
                jnp.concatenate(weights, axis=1),
                jnp.concatenate([values, ones], axis=1),
                preferred_element_type=jnp.float32,
            )
            if carried:
                fade = jnp.exp2((top_in - top) * scale)
                out = out + jnp.concatenate([fade, fade], axis=1) * acc_old[b, :, both]
            if final:
                out_ref[:, cols] = (out[:, :HD] * (1.0 / out[:, HD:])).astype(jnp.bfloat16)
            else:
                outs[0][b, :, both] = out
                outs[1][b, :, cols] = top

    if final:
        for b in range(*qs):
            one(b, outs[b - qs[0]])
    else:
        pl.loop(*qs)(lambda b: one(b, None))


def attend(held, state, qs, keys, carried, final, n_q, group):
    query, key, value = held
    n_all, rows, _ = query.shape
    n_kv = key.shape[2] // HD
    vmem = pl.BlockSpec(memory_space=pltpu.VMEM)
    args, in_specs, aliases = [query, key, value], [vmem] * 3, {}
    if state is not None and (carried or not final):
        in_specs += [vmem if carried else ANY] * 2
        args += list(state)
    if final:
        out_shape = [jax.ShapeDtypeStruct((rows, n_q * HD), jnp.bfloat16)] * (qs[1] - qs[0])
    else:
        out_shape = [
            jax.ShapeDtypeStruct((n_all, rows, 2 * n_q * HD), jnp.float32),
            jax.ShapeDtypeStruct((n_all, rows, n_q * HD), jnp.float32),
        ]
        if state is not None:
            aliases = {3: 0, 4: 1}
    n_pairs = (qs[1] - qs[0]) * (keys[1] - keys[0])
    return pl.pallas_call(
        functools.partial(attend_kernel, n_q, group, qs, keys, carried, final),
        out_shape=out_shape,
        in_specs=in_specs,
        out_specs=[vmem] * len(out_shape),
        input_output_aliases=aliases,
        cost_estimate=pl.CostEstimate(
            flops=16 * n_pairs * rows * rows * n_q * HD,
            bytes_accessed=2 * (qs[1] - qs[0]) * rows * (2 * n_q + 2 * n_kv) * HD,
            transcendentals=n_pairs * rows * rows * n_q,
        ),
        compiler_params=params(24),
        name="attend",
    )(*args)


def mix_kernel(places, n_s, n_w, n_y, n_d, arranged, index_ref, *refs):
    w_refs, refs = refs[:n_w], refs[n_w:]
    depth, wide = w_refs[0].shape[-2:]
    if arranged:
        a_ref, (out_ref, o_held, sem) = refs[0], refs[-3:]
    else:
        out_ref, a_ref, o_held, sem, a_held = refs[-5:]
        part = refs[0].shape[1]
        many = depth // part
        for s in range(n_s):
            a_held[index_ref[n_d + 2 * n_s + s]] = refs[s][...]
        for d in range(n_d):
            for p in range(many):
                at = d * depth + p * part
                a_ref[:, at : at + part] = a_held[index_ref[d] * many + p]
    copies = []
    for n, (i, j) in enumerate(sorted({(i, j) for i, j, _ in places})):
        total = None
        for d in range(n_d):
            t, plane = places[i, j, d]
            lhs = a_ref[:, d * depth : (d + 1) * depth]
            term = jnp.dot(lhs, w_refs[t][plane], preferred_element_type=jnp.float32)
            total = term if total is None else total + term
        o_held[n] = total.astype(jnp.bfloat16)
        at = pl.multiple_of(index_ref[n_d + i * n_y + j] * wide, wide)
        copies.append(pltpu.make_async_copy(o_held.at[n], out_ref.at[:, pl.ds(at, wide)], sem.at[n]))
        copies[-1].start()
    for copy in copies:
        copy.wait()


def mix(heads, pieces, places, index, n_s, n_y, n_d, so_far):
    arranged = so_far is not None
    rows, part = heads[0].shape
    part = part // n_s if arranged else part
    wide = pieces[0].shape[2]
    n_w, n_cols = len(pieces), len(places) // n_d
    vmem = pl.BlockSpec(memory_space=pltpu.VMEM)
    args = [index, *pieces, *heads]
    in_specs = [pl.BlockSpec(memory_space=pltpu.SMEM)] + [vmem] * (len(args) - 1)
    out_shape = [jax.ShapeDtypeStruct((rows, n_s * wide), jnp.bfloat16)]
    scratch = [pltpu.VMEM((n_cols, rows, wide), jnp.bfloat16), pltpu.SemaphoreType.DMA((n_cols,))]
    aliases = {}
    if arranged:
        aliases = {len(args): 0}
        args.append(so_far)
        in_specs.append(ANY)
    else:
        out_shape.append(jax.ShapeDtypeStruct((rows, n_s * part), jnp.bfloat16))
        scratch.append(pltpu.VMEM((n_s, rows, part), jnp.bfloat16))
    return pl.pallas_call(
        functools.partial(mix_kernel, places, n_s, n_w, n_y, n_d, arranged),
        out_shape=out_shape,
        in_specs=in_specs,
        out_specs=[ANY] + [vmem] * (len(out_shape) - 1),
        input_output_aliases=aliases,
        scratch_shapes=scratch,
        cost_estimate=pl.CostEstimate(
            flops=2 * rows * n_s * part * n_cols * wide,
            bytes_accessed=2 * n_s * part * n_cols * wide,
            transcendentals=0,
        ),
        compiler_params=params(16),
        name="mix",
    )(*args)


def layout(n_sp, n_dp):
    n_z, n_c = math.gcd(n_sp, 4), math.gcd(n_dp, 2)
    return n_z, n_sp // n_z, n_dp // n_c, n_c


def on_device(tokens, w_query, w_key, w_value, w_out, qk_gain):
    own_rows = tokens[0]
    rows, depth = own_rows.shape
    n_sp, n_dp = lax.axis_size("sp"), lax.axis_size("dp")
    seq_len = rows * n_sp
    n_z, n_y, n_x, n_c = layout(n_sp, n_dp)
    n_q = HQ // n_sp
    group = HQ // KV
    share = max(1, n_sp // KV)
    if share > 1:
        groups = [[g * share + i for i in range(share)] for g in range(n_sp // share)]
        whole_head = lambda w: lax.all_gather(w, "sp", axis=1, axis_index_groups=groups, tiled=True)
        w_key, w_value = whole_head(w_key), whole_head(w_value)
    n_kv = w_key.shape[1] // HD
    d_slots = [(i, 0) for i in range(n_x)] + [(i, j) for i in range(n_x) for j in range(1, n_c)]
    s_slots = [(i, j) for i in range(n_z) for j in range(n_y)]
    n_d = len(d_slots)
    last = n_z + n_y - 2
    order = sorted(s_slots, key=lambda s: max(sum(s), 1))
    s_owner = {s: owner_of("sp", n_z, n_y, *s) for s in s_slots}
    index = jnp.stack(
        [owner_of("dp", n_x, n_c, *s) for s in d_slots]
        + [s_owner[s] for s in s_slots]
        + [s_owner[s] for s in order]
        + [owner_of("sp", n_z, n_y, n_z - i, n_y - j) for i, j in order]
    ).astype(jnp.int32)
    up_z, up_y = shift(n_z, n_y, True), shift(n_z, n_y, False)
    up_x, up_c = shift(n_x, n_c, True), shift(n_x, n_c, False)

    cut = rows // 2
    blocks = {(0, 0): [own_rows]}
    for j in range(1, n_y):
        blocks[0, j] = [lax.ppermute(blocks[0, j - 1][0], "sp", up_y)]
    half0 = lax.optimization_barrier(own_rows)[:cut]
    half1 = lax.optimization_barrier(own_rows)[cut:]
    column = [half0, half1]
    for i in range(1, n_z):
        column = blocks[i, 0] = [lax.ppermute(b, "sp", up_z) for b in column]
        for j in range(1, n_y):
            along = list(blocks[i, j - 1])
            if (i, j) == (n_z - 1, n_y - 1):
                along[-1] = along[-1][: cut // 2]
            blocks[i, j] = [lax.ppermute(b, "sp", up_y) for b in along]
    if n_y > 1:
        quarter = blocks[0, n_y - 1][0][rows - (cut - cut // 2) :]
        blocks[n_z - 1, n_y - 1].append(lax.ppermute(quarter, "sp", send_back(n_z, n_y, 1, 0)))

    w_blocks = {(0, 0): jnp.concatenate([w_query, w_key, w_value], axis=1)}
    for i in range(1, n_x):
        w_blocks[i, 0] = lax.ppermute(w_blocks[i - 1, 0], "dp", up_x)
    for i in range(n_x):
        for j in range(1, n_c):
            w_blocks[i, j] = lax.ppermute(w_blocks[i, j - 1], "dp", up_c)
    weight = assemble(
        [w_blocks[s] for s in d_slots],
        [(b, None, b, None) for b in range(n_d)],
        index,
        (depth, w_blocks[0, 0].shape[1]),
    )
    tables = rotary_tables(seq_len)

    held = state = None
    n_held = n_done = 0
    for turn in range(1, last + 1):
        ready = [s for s in order if max(sum(s), 1) == turn]
        held = project(
            [blocks[s] for s in ready], [s_slots.index(s) for s in ready], n_held, weight, index, n_d,
            qk_gain, *tables, n_q, n_kv, held, n_sp,
        )
        n_held += len(ready)
        old, final = (0, n_done), turn == last
        fresh = (n_done, n_held)
        carry = functools.partial(attend, n_q=n_q, group=group)
        if n_done:
            updated = carry(held, state, old, fresh, True, final)
            state = state if final else updated
        made = carry(held, state, fresh, (0, n_held), False, final)
        if final:
            attended = [*updated, *made]
        else:
            state = made
        n_done = n_held
    heads = []
    for (i, j), block in zip(order, attended):
        if i or j:
            block = lax.ppermute(block, "sp", send_back(n_z, n_y, i, j))
        heads.append(block)

    ring = [w_out]
    for _ in range(1, n_z):
        ring.append(lax.ppermute(ring[-1], "sp", up_z))
    first = range((n_z + 1) // 2)
    parts = [first] + [[i] for i in range(len(first), n_z)]
    pieces, places = [], {}
    for part in parts:
        column = jnp.stack([ring[i] for i in part])
        for j in range(n_y):
            if j:
                column = lax.ppermute(column, "sp", up_y)
            row = column
            for i in range(n_x):
                if i:
                    row = lax.ppermute(row, "dp", up_x)
                piece = row
                for c in range(n_c):
                    if c:
                        piece = lax.ppermute(piece, "dp", up_c)
                    for p, z_slot in enumerate(part):
                        places[z_slot, j, d_slots.index((i, c))] = len(pieces), p
                    pieces.append(piece)
    out = None
    group_of = lambda i, j: 0 if j < n_y - 1 else 1 if i < n_z - 1 else 2
    for n in range(3):
        mine = {place: at for place, at in places.items() if group_of(*place[:2]) == n}
        if not mine:
            continue
        used = sorted({t for t, _ in mine.values()})
        mine = {place: (used.index(t), p) for place, (t, p) in mine.items()}
        out, *arranged = mix(heads, [pieces[t] for t in used], mine, index, n_sp, n_y, n_d, out)
        heads = arranged or heads
    return out[None]


def solution(mesh):
    in_specs = (
        P("dp", "sp", None),
        P("dp", "sp"),
        P("dp", "sp"),
        P("dp", "sp"),
        P("dp", "sp"),
        P(),
    )
    out_specs = P("dp", "sp", None)

    return jax.shard_map(
        on_device, mesh=mesh, in_specs=in_specs, out_specs=out_specs, check_vma=False
    )
```

```python
import functools
import math

import jax
import jax.numpy as jnp
from jax import lax
from jax.experimental import pallas as pl
from jax.experimental.pallas import tpu as pltpu
from jax.sharding import PartitionSpec as P


HQ = 16
KV = 8
HD = 128
GRID_W = 64

ROPE_BASE = 10000.0
EPS = 1e-06
LOG2E = 1.4426950408889634


def rotary_tables(seq_len):
    positions = jnp.arange(seq_len, dtype=jnp.int32)
    quarter = jnp.arange(0, HD // 2, 2, dtype=jnp.float32)
    inv_freq = jnp.repeat(ROPE_BASE ** (-quarter / (HD // 2)), 2)
    row_pos = (positions // GRID_W).astype(jnp.float32)
    col_pos = (positions % GRID_W).astype(jnp.float32)
    angle = jnp.concatenate([row_pos[:, None] * inv_freq, col_pos[:, None] * inv_freq], axis=1)
    sign = jnp.where(jnp.arange(HD) % 2 == 0, -1.0, 1.0).astype(jnp.float32)
    return jnp.cos(angle), jnp.sin(angle) * sign


def shift(n_outer, n_inner, outer):
    pairs = []
    for a in range(n_outer):
        for b in range(n_inner):
            to = ((a + 1) % n_outer, b) if outer else (a, (b + 1) % n_inner)
            pairs.append((a * n_inner + b, to[0] * n_inner + to[1]))
    return pairs


def send_back(n_outer, n_inner, i, j):
    return [
        (a * n_inner + b, (a - i) % n_outer * n_inner + (b - j) % n_inner)
        for a in range(n_outer)
        for b in range(n_inner)
    ]


def owner_of(axis, n_outer, n_inner, i, j):
    me = lax.axis_index(axis)
    return lax.rem(me // n_inner + 2 * n_outer - i, n_outer) * n_inner + lax.rem(
        lax.rem(me, n_inner) + 2 * n_inner - j, n_inner
    )


def whole(shape):
    return pl.BlockSpec(shape, lambda i, ix: (0,) * len(shape))


ANY = pl.BlockSpec(memory_space=pl.ANY)


def params(mib):
    return pltpu.CompilerParams(vmem_limit_bytes=mib * 2**20)


def assemble_kernel(places, index_ref, *refs):
    block_refs, (out_ref, sem) = refs[:-2], refs[-2:]
    copies = []
    for t, (b, lead, row, col) in enumerate(places):
        src = block_refs[b] if lead is None else block_refs[b].at[lead]
        height, width = src.shape
        to = out_ref
        if row is not None:
            to = to.at[pl.ds(pl.multiple_of(index_ref[row] * height, height), height)]
        if col is not None:
            to = to.at[:, pl.ds(pl.multiple_of(index_ref[col] * width, width), width)]
        copies.append(pltpu.make_async_copy(src, to, sem.at[t]))
        copies[-1].start()
    for copy in copies:
        copy.wait()


def assemble(blocks, places, index, shape):
    return pl.pallas_call(
        functools.partial(assemble_kernel, places),
        out_shape=jax.ShapeDtypeStruct(shape, jnp.bfloat16),
        grid_spec=pltpu.PrefetchScalarGridSpec(
            num_scalar_prefetch=1,
            grid=(1,),
            in_specs=[ANY] * len(blocks),
            out_specs=whole(shape),
            scratch_shapes=[pltpu.SemaphoreType.DMA((len(places),))],
        ),
        cost_estimate=pl.CostEstimate(
            flops=1000 * math.prod(shape), bytes_accessed=4 * math.prod(shape), transcendentals=0
        ),
        compiler_params=params(8),
        name="assemble",
    )(index, *blocks)


def project_kernel(n_b, n_x, n_q, n_kv, first, index_ref, *refs):
    x_refs, refs = refs[:n_x], refs[n_x:]
    cos_refs, refs = refs[:n_b], refs[n_b:]
    sin_refs, refs = refs[:n_b], refs[n_b:]
    gain_ref, w_ref = refs[:2]
    outs, held, x_whole, x_sem, sem = refs[-9:-6], refs[-6:-3], refs[-3], refs[-2], refs[-1]
    q_ref, k_ref, v_ref = held
    loads, ends, at = [], [], 0
    for t in range(n_x):
        height = x_refs[t].shape[0]
        loads.append(pltpu.make_async_copy(x_refs[t], x_whole.at[pl.ds(at, height)], x_sem.at[t]))
        loads[-1].start()
        at += height
        ends.append(at)
    q_width, kv_width = n_q * HD, n_kv * HD
    even = lax.broadcasted_iota(jnp.int32, cos_refs[0].shape, 1) % 2 == 0
    rows = q_ref.shape[1]
    copies = []
    for b in range(n_b):
        while ends and ends[0] <= (b + 1) * rows:
            ends.pop(0)
            loads.pop(0).wait()
        x = x_whole[b * rows : (b + 1) * rows, :]
        total = jnp.dot(x, w_ref[...], preferred_element_type=jnp.float32)
        cos, sin = cos_refs[b][...], sin_refs[b][...]

        def turned(raw, gain):
            normed = raw * lax.rsqrt(jnp.mean(raw * raw, axis=-1, keepdims=True) + EPS) * gain
            other = jnp.where(even, pltpu.roll(normed, HD - 1, 1), pltpu.roll(normed, 1, 1))
            return (normed * cos + other * sin).astype(jnp.bfloat16)

        for h in range(n_q):
            at = h * HD
            q_ref[b, :, at : at + HD] = turned(total[:, at : at + HD], gain_ref[0:1, :])
        for h in range(n_kv):
            at = h * HD
            raw = total[:, q_width + at : q_width + at + HD]
            k_ref[b, :, at : at + HD] = turned(raw, gain_ref[1:2, :])
        v_ref[b] = total[:, q_width + kv_width :].astype(jnp.bfloat16)
    for i in range(3):
        copies.append(pltpu.make_async_copy(held[i], outs[i].at[pl.ds(first, n_b)], sem.at[i]))
        copies[-1].start()
    for copy in copies:
        copy.wait()


def project(blocks, slots, first, weight, index, n_d, gain, cos, sin, n_q, n_kv, held, n_all):
    halves = [half for block in blocks for half in block]
    n_b, n_x = len(blocks), len(halves)
    depth = halves[0].shape[1]
    rows = sum(half.shape[0] for half in halves) // n_b
    width = weight.shape[1]
    at_rows = [pl.BlockSpec((rows, HD), lambda i, ix, s=s: (ix[n_d + s], 0)) for s in slots]
    in_specs = [ANY] * n_x + at_rows + at_rows + [whole(gain.shape), whole(weight.shape)]
    args = [*halves, *[cos] * n_b, *[sin] * n_b, gain, weight]
    aliases = {}
    if held is not None:
        aliases = {1 + len(args) + i: i for i in range(3)}
        in_specs += [ANY] * 3
        args += list(held)
    widths = (n_q * HD, n_kv * HD, n_kv * HD)
    return pl.pallas_call(
        functools.partial(project_kernel, n_b, n_x, n_q, n_kv, first),
        out_shape=[jax.ShapeDtypeStruct((n_all, rows, w), jnp.bfloat16) for w in widths],
        grid_spec=pltpu.PrefetchScalarGridSpec(
            num_scalar_prefetch=1,
            grid=(1,),
            in_specs=in_specs,
            out_specs=[ANY] * 3,
            scratch_shapes=[pltpu.VMEM((n_b, rows, w), jnp.bfloat16) for w in widths]
            + [
                pltpu.VMEM((n_b * rows, depth), jnp.bfloat16),
                pltpu.SemaphoreType.DMA((n_x,)),
                pltpu.SemaphoreType.DMA((3,)),
            ],
        ),
        input_output_aliases=aliases,
        cost_estimate=pl.CostEstimate(
            flops=4 * n_b * rows * depth * width,
            bytes_accessed=2 * (n_b * rows * depth + depth * width + n_b * rows * width),
            transcendentals=0,
        ),
        compiler_params=params(20),
        name="project",
    )(index, *args)


def attend_kernel(n_q, group, qs, keys, carried, final, q_ref, k_ref, v_ref, *refs):
    if carried:
        acc_old, top_old = refs[:2]
    outs = refs[-(qs[1] - qs[0]) :] if final else refs[-2:]
    rows = q_ref.shape[1]
    scale = HD**-0.5 * LOG2E

    n_keys = (keys[1] - keys[0]) * rows
    ones = jnp.ones((n_keys, HD), jnp.bfloat16)

    def one(b, out_ref):
        for h in range(n_q):
            at = (h // group) * HD
            cols = slice(h * HD, (h + 1) * HD)
            both = slice(2 * h * HD, 2 * (h + 1) * HD)
            some = k_ref[keys[0] : keys[1], :, at : at + HD].reshape(n_keys, HD)
            values = v_ref[keys[0] : keys[1], :, at : at + HD].reshape(n_keys, HD)
            scores = lax.dot_general(
                q_ref[b, :, cols], some, (((1,), (1,)), ((), ())), preferred_element_type=jnp.float32
            )
            top = jnp.broadcast_to(jnp.max(scores, axis=1, keepdims=True), (rows, HD))
            if carried:
                top_in = top_old[b, :, cols]
                top = jnp.maximum(top, top_in)
            weights = [
                jnp.exp2((scores[:, c : c + HD] - top) * scale).astype(jnp.bfloat16)
                for c in range(0, n_keys, HD)
            ]
            out = jnp.dot(
                jnp.concatenate(weights, axis=1),
                jnp.concatenate([values, ones], axis=1),
                preferred_element_type=jnp.float32,
            )
            if carried:
                fade = jnp.exp2((top_in - top) * scale)
                out = out + jnp.concatenate([fade, fade], axis=1) * acc_old[b, :, both]
            if final:
                out_ref[:, cols] = (out[:, :HD] * (1.0 / out[:, HD:])).astype(jnp.bfloat16)
            else:
                outs[0][b, :, both] = out
                outs[1][b, :, cols] = top

    if final:
        for b in range(*qs):
            one(b, outs[b - qs[0]])
    else:
        pl.loop(*qs)(lambda b: one(b, None))


def attend(held, state, qs, keys, carried, final, n_q, group):
    query, key, value = held
    n_all, rows, _ = query.shape
    n_kv = key.shape[2] // HD
    vmem = pl.BlockSpec(memory_space=pltpu.VMEM)
    args, in_specs, aliases = [query, key, value], [vmem] * 3, {}
    if state is not None and (carried or not final):
        in_specs += [vmem if carried else ANY] * 2
        args += list(state)
    if final:
        out_shape = [jax.ShapeDtypeStruct((rows, n_q * HD), jnp.bfloat16)] * (qs[1] - qs[0])
    else:
        out_shape = [
            jax.ShapeDtypeStruct((n_all, rows, 2 * n_q * HD), jnp.float32),
            jax.ShapeDtypeStruct((n_all, rows, n_q * HD), jnp.float32),
        ]
        if state is not None:
            aliases = {3: 0, 4: 1}
    n_pairs = (qs[1] - qs[0]) * (keys[1] - keys[0])
    return pl.pallas_call(
        functools.partial(attend_kernel, n_q, group, qs, keys, carried, final),
        out_shape=out_shape,
        in_specs=in_specs,
        out_specs=[vmem] * len(out_shape),
        input_output_aliases=aliases,
        cost_estimate=pl.CostEstimate(
            flops=16 * n_pairs * rows * rows * n_q * HD,
            bytes_accessed=2 * (qs[1] - qs[0]) * rows * (2 * n_q + 2 * n_kv) * HD,
            transcendentals=n_pairs * rows * rows * n_q,
        ),
        compiler_params=params(24),
        name="attend",
    )(*args)


def mix_kernel(places, n_s, n_w, n_y, n_d, arranged, index_ref, *refs):
    w_refs, refs = refs[:n_w], refs[n_w:]
    depth, wide = w_refs[0].shape[-2:]
    if arranged:
        a_ref, (out_ref, o_held, sem) = refs[0], refs[-3:]
    else:
        out_ref, a_ref, o_held, sem, a_held = refs[-5:]
        part = refs[0].shape[1]
        many = depth // part
        for s in range(n_s):
            a_held[index_ref[n_d + 2 * n_s + s]] = refs[s][...]
        for d in range(n_d):
            for p in range(many):
                at = d * depth + p * part
                a_ref[:, at : at + part] = a_held[index_ref[d] * many + p]
    copies = []
    for n, (i, j) in enumerate(sorted({(i, j) for i, j, _ in places})):
        total = None
        for d in range(n_d):
            t, plane = places[i, j, d]
            lhs = a_ref[:, d * depth : (d + 1) * depth]
            term = jnp.dot(lhs, w_refs[t][plane], preferred_element_type=jnp.float32)
            total = term if total is None else total + term
        o_held[n] = total.astype(jnp.bfloat16)
        at = pl.multiple_of(index_ref[n_d + i * n_y + j] * wide, wide)
        copies.append(pltpu.make_async_copy(o_held.at[n], out_ref.at[:, pl.ds(at, wide)], sem.at[n]))
        copies[-1].start()
    for copy in copies:
        copy.wait()


def mix(heads, pieces, places, index, n_s, n_y, n_d, so_far):
    arranged = so_far is not None
    rows, part = heads[0].shape
    part = part // n_s if arranged else part
    wide = pieces[0].shape[2]
    n_w, n_cols = len(pieces), len(places) // n_d
    vmem = pl.BlockSpec(memory_space=pltpu.VMEM)
    args = [index, *pieces, *heads]
    in_specs = [pl.BlockSpec(memory_space=pltpu.SMEM)] + [vmem] * (len(args) - 1)
    out_shape = [jax.ShapeDtypeStruct((rows, n_s * wide), jnp.bfloat16)]
    scratch = [pltpu.VMEM((n_cols, rows, wide), jnp.bfloat16), pltpu.SemaphoreType.DMA((n_cols,))]
    aliases = {}
    if arranged:
        aliases = {len(args): 0}
        args.append(so_far)
        in_specs.append(ANY)
    else:
        out_shape.append(jax.ShapeDtypeStruct((rows, n_s * part), jnp.bfloat16))
        scratch.append(pltpu.VMEM((n_s, rows, part), jnp.bfloat16))
    return pl.pallas_call(
        functools.partial(mix_kernel, places, n_s, n_w, n_y, n_d, arranged),
        out_shape=out_shape,
        in_specs=in_specs,
        out_specs=[ANY] + [vmem] * (len(out_shape) - 1),
        input_output_aliases=aliases,
        scratch_shapes=scratch,
        cost_estimate=pl.CostEstimate(
            flops=2 * rows * n_s * part * n_cols * wide,
            bytes_accessed=2 * n_s * part * n_cols * wide,
            transcendentals=0,
        ),
        compiler_params=params(16),
        name="mix",
    )(*args)


def layout(n_sp, n_dp):
    n_z, n_c = math.gcd(n_sp, 4), math.gcd(n_dp, 2)
    return n_z, n_sp // n_z, n_dp // n_c, n_c


def on_device(tokens, w_query, w_key, w_value, w_out, qk_gain):
    own_rows = tokens[0]
    rows, depth = own_rows.shape
    n_sp, n_dp = lax.axis_size("sp"), lax.axis_size("dp")
    seq_len = rows * n_sp
    n_z, n_y, n_x, n_c = layout(n_sp, n_dp)
    n_q = HQ // n_sp
    group = HQ // KV
    share = max(1, n_sp // KV)
    if share > 1:
        groups = [[g * share + i for i in range(share)] for g in range(n_sp // share)]
        whole_head = lambda w: lax.all_gather(w, "sp", axis=1, axis_index_groups=groups, tiled=True)
        w_key, w_value = whole_head(w_key), whole_head(w_value)
    n_kv = w_key.shape[1] // HD
    d_slots = [(i, 0) for i in range(n_x)] + [(i, j) for i in range(n_x) for j in range(1, n_c)]
    s_slots = [(i, j) for i in range(n_z) for j in range(n_y)]
    n_d = len(d_slots)
    last = n_z + n_y - 2
    stages = [[s for s in s_slots if max(sum(s), 1) == turn] for turn in range(1, last + 1)]
    if last > 2:
        late = sorted(stages[-2], key=lambda s: s[0])
        stages[-2:-1] = [late[:-1], late[-1:]]
    order = sum(stages, [])
    s_owner = {s: owner_of("sp", n_z, n_y, *s) for s in s_slots}
    index = jnp.stack(
        [owner_of("dp", n_x, n_c, *s) for s in d_slots]
        + [s_owner[s] for s in s_slots]
        + [s_owner[s] for s in order]
        + [owner_of("sp", n_z, n_y, n_z - i, n_y - j) for i, j in order]
    ).astype(jnp.int32)
    up_z, up_y = shift(n_z, n_y, True), shift(n_z, n_y, False)
    up_x, up_c = shift(n_x, n_c, True), shift(n_x, n_c, False)

    cut = rows // 2
    blocks = {(0, 0): [own_rows]}
    for j in range(1, n_y):
        blocks[0, j] = [lax.ppermute(blocks[0, j - 1][0], "sp", up_y)]
    half0 = lax.optimization_barrier(own_rows)[:cut]
    half1 = lax.optimization_barrier(own_rows)[cut:]
    column = [half0, half1]
    for i in range(1, n_z):
        column = blocks[i, 0] = [lax.ppermute(b, "sp", up_z) for b in column]
        for j in range(1, n_y):
            along = list(blocks[i, j - 1])
            if (i, j) == (n_z - 1, n_y - 1):
                along[-1] = along[-1][: cut // 2]
            blocks[i, j] = [lax.ppermute(b, "sp", up_y) for b in along]
    if n_y > 1:
        quarter = blocks[0, n_y - 1][0][rows - (cut - cut // 2) :]
        blocks[n_z - 1, n_y - 1].append(lax.ppermute(quarter, "sp", send_back(n_z, n_y, 1, 0)))

    w_blocks = {(0, 0): jnp.concatenate([w_query, w_key, w_value], axis=1)}
    for i in range(1, n_x):
        w_blocks[i, 0] = lax.ppermute(w_blocks[i - 1, 0], "dp", up_x)
    for i in range(n_x):
        for j in range(1, n_c):
            w_blocks[i, j] = lax.ppermute(w_blocks[i, j - 1], "dp", up_c)
    weight = assemble(
        [w_blocks[s] for s in d_slots],
        [(b, None, b, None) for b in range(n_d)],
        index,
        (depth, w_blocks[0, 0].shape[1]),
    )
    tables = rotary_tables(seq_len)

    held = state = None
    n_held = n_done = 0
    for turn, ready in enumerate(stages, 1):
        held = project(
            [blocks[s] for s in ready], [s_slots.index(s) for s in ready], n_held, weight, index, n_d,
            qk_gain, *tables, n_q, n_kv, held, n_sp,
        )
        n_held += len(ready)
        old, final = (0, n_done), turn == len(stages)
        fresh = (n_done, n_held)
        carry = functools.partial(attend, n_q=n_q, group=group)
        if n_done:
            updated = carry(held, state, old, fresh, True, final)
            state = state if final else updated
        made = carry(held, state, fresh, (0, n_held), False, final)
        if final:
            attended = [*updated, *made]
        else:
            state = made
        n_done = n_held
    heads = []
    for (i, j), block in zip(order, attended):
        if i or j:
            block = lax.ppermute(block, "sp", send_back(n_z, n_y, i, j))
        heads.append(block)

    ring = [w_out]
    for _ in range(1, n_z):
        ring.append(lax.ppermute(ring[-1], "sp", up_z))
    first = range((n_z + 1) // 2)
    parts = [first] + [[i] for i in range(len(first), n_z)]
    pieces, places = [], {}
    for part in parts:
        column = jnp.stack([ring[i] for i in part])
        for j in range(n_y):
            if j:
                column = lax.ppermute(column, "sp", up_y)
            row = column
            for i in range(n_x):
                if i:
                    row = lax.ppermute(row, "dp", up_x)
                piece = row
                for c in range(n_c):
                    if c:
                        piece = lax.ppermute(piece, "dp", up_c)
                    for p, z_slot in enumerate(part):
                        places[z_slot, j, d_slots.index((i, c))] = len(pieces), p
                    pieces.append(piece)
    out = None
    group_of = lambda i, j: 0 if j < n_y - 1 else 1 if i < n_z - 1 else 2
    for n in range(3):
        mine = {place: at for place, at in places.items() if group_of(*place[:2]) == n}
        if not mine:
            continue
        used = sorted({t for t, _ in mine.values()})
        mine = {place: (used.index(t), p) for place, (t, p) in mine.items()}
        out, *arranged = mix(heads, [pieces[t] for t in used], mine, index, n_sp, n_y, n_d, out)
        heads = arranged or heads
    return out[None]


def solution(mesh):
    in_specs = (
        P("dp", "sp", None),
        P("dp", "sp"),
        P("dp", "sp"),
        P("dp", "sp"),
        P("dp", "sp"),
        P(),
    )
    out_specs = P("dp", "sp", None)

    return jax.shard_map(
        on_device, mesh=mesh, in_specs=in_specs, out_specs=out_specs, check_vma=False
    )
```
